32 devices in a mesh: sp: 8 (over z, x), tp: 4 (over y, core).
Axes of the slice: x: 2, y: 2, z: 4, core: 2. Of those that a mesh axis runs over, the one named last changes fastest.
Arguments:
- layer_input: bfloat16 [1024, 2048], P('sp'), may hold values from -6 to 6
- out_cot: bfloat16 [1024, 2048], P('sp'), may hold values from -6 to 6
- routes: int32 [1024, 2], P('sp'), may hold values from 0 to 7, all different within a row; in each aligned block of 128 rows (0 to 127, 128 to 255, ...) at most 64 rows name the same one
- route_weights: float32 [1024, 2], P('sp'), may hold values from 0.2 to 1
- gate_weights: bfloat16 [8, 2048, 1024], P('sp', None, 'tp'), may hold values from -0.125 to 0.125
- up_weights: bfloat16 [8, 2048, 1024], P('sp', None, 'tp'), may hold values from -0.125 to 0.125
- down_weights: bfloat16 [8, 1024, 2048], P('sp', 'tp'), may hold values from -0.1875 to 0.1875
- out_proj: bfloat16 [2048, 2048], P(None, 'tp'), may hold values from -0.125 to 0.125
- queries: bfloat16 [1024, 2048], P('sp', 'tp'), may hold values from -6 to 6
- keys: bfloat16 [1024, 2048], P('sp', 'tp'), may hold values from -6 to 6
- values: bfloat16 [1024, 2048], P('sp', 'tp'), may hold values from -6 to 6
- mixer_out: bfloat16 [1024, 2048], P('sp', 'tp'), may hold values from -6 to 6
- entry_states: float32 [8, 32, 64, 64], P('sp', 'tp'), may hold values from -6 to 6
Outputs:
- grad_gate: bfloat16 [8, 2048, 1024], P('sp', None, 'tp')
- grad_up: bfloat16 [8, 2048, 1024], P('sp', None, 'tp')
- grad_down: bfloat16 [8, 1024, 2048], P('sp', 'tp')
- grad_proj: float32 [2048, 2048], P('sp', 'tp')
- grad_queries: bfloat16 [1024, 2048], P('sp', 'tp')
- grad_keys: bfloat16 [1024, 2048], P('sp', 'tp')
- grad_values: bfloat16 [1024, 2048], P('sp', 'tp')
The draws below stay inside these ranges and needn't reach their ends.
Inputs may be any that keep to these rules, and one draw needn't show every extreme that they name: `routes`: in each aligned block of 128 rows no expert is named by more than 64 rows, a bound that some block reaches; the numbers of one row differ.
All inputs are finite; a program needn't handle non-finite values.
Results may differ from the reference program's by a relative error of at most 0.01.
Values may be sent and summed in bfloat16 or wider, within the bound.
A program may use at most 128 MiB of HBM per device.

```python
import math
import jax
import jax.numpy as jnp
import numpy as np
from jax import lax

D = 2048
FF = 1024
HEADS = 32
DK = 64
TOPK = 2
SPAN = 128
TOK_DEV = 128
TOKENS = 1024
EXPERTS = 8
CAP = 64
HV = 2048
N_SP = 8


def raised(array, stream_key, source, target, shards_of, factor):
    def block_of(dim):
        return (jnp.arange(array.shape[dim]) // (array.shape[dim] // shards_of)).reshape((-1,) + (1,) * (array.ndim - 1 - dim))

    near = jax.random.permutation(stream_key, shards_of)[block_of(target)]
    far = (block_of(target) + shards_of // 2) % shards_of
    return jnp.where((block_of(source) == near) | (block_of(source) == far), factor * array, array)


def block_levels(rng, extent, split, smallest, high):
    level, own = 1.0, jax.random.fold_in(rng, 6)
    for axis_at, parts in split:
        heights = jnp.exp(jax.random.uniform(jax.random.fold_in(own, axis_at), (parts,), jnp.float32, smallest / len(split), high / len(split)))
        level = level * jnp.repeat(heights, extent[axis_at] // parts).reshape([-1 if axis == axis_at else 1 for axis in range(len(extent))])
    return level


def routed_block(rng, own, number, rows, amount, top, limit, lean):
    sequence = jax.random.permutation(rng, amount)
    heavy_load, common = shares(amount, rows * top, limit, lean, True), shares(amount, rows * top, limit, lean, False)
    places = jnp.arange(amount)

    def named(tallies, turn):
        used = int((tallies > 0).sum())
        fixed = max(1, used // 4)
        moved = fixed + (places - fixed + turn * (used - fixed)) % max(1, amount - fixed)
        return jnp.zeros((amount,), jnp.int32).at[sequence[jnp.where(places < fixed, places, moved)]].set(jnp.asarray(tallies, jnp.int32))

    tallies = jnp.where(number % 4 == 0, named(heavy_load, number // 4), named(common, number - number // 4 - 1))
    mixed = jax.random.permutation(jax.random.fold_in(own, 3), amount)
    donor, receiver = mixed[0:amount // 2 * 2:2], mixed[1:amount // 2 * 2:2]
    slack = jnp.minimum(tallies[donor] - 1, limit - tallies[receiver]) // 2
    slack = jnp.where((donor == sequence[0]) | (receiver == sequence[0]) | (tallies[receiver] == 0), 0, jnp.maximum(slack, 0))
    moved = jax.random.randint(jax.random.fold_in(own, 4), (amount // 2,), 0, 1 << 20) % (slack + 1)
    tallies = tallies.at[donor].add(-moved).at[receiver].add(moved)
    members = jnp.searchsorted(jnp.cumsum(tallies), jnp.arange(rows * top), side="right").astype(jnp.int32)
    listing = members.reshape(top, rows).T
    listing = listing[jax.random.permutation(jax.random.fold_in(own, 1), rows)]
    turn = jax.random.randint(jax.random.fold_in(own, 2), (rows, 1), 0, top)
    return jnp.take_along_axis(listing, (jnp.arange(top)[None, :] + turn) % top, axis=1)


def shares(number_of, total, bound, skew, full):
    weights = [(1 << 20) // math.isqrt(grade ** skew) + 1 for grade in range(1, number_of + 1)]
    largest = bound if full else min(bound, max(-(-total // number_of), total * weights[0] // sum(weights)))
    least = 1 if total - largest >= number_of - 1 else 0
    counts, surplus = [largest] + [least] * (number_of - 1), total - largest - least * (number_of - 1)
    while surplus > 0:
        candidates = [i for i in range(1, number_of) if counts[i] < largest] or [i for i in range(1, number_of) if counts[i] < bound]
        whole, left = sum([weights[i] for i in candidates]), surplus
        for i in candidates:
            more = min(bound - counts[i], max(1, left * weights[i] // whole), surplus)
            counts[i] = counts[i] + more
            surplus = surplus - more
    return np.array(counts)


def noise(rng, shape, spread, limit, pieces=(), kind=jnp.bfloat16):
    drawn = jax.random.normal(rng, shape, jnp.float32) * spread
    if len(pieces) > 0:
        drawn = block_levels(rng, shape, pieces, -0.22, 0.18) * drawn
    return jnp.clip(drawn, min=-limit, max=limit).astype(kind)


def bell_draw_with(key, shape, scale, limit, split, heavy, held_as=jnp.bfloat16):
    values = scale * jax.random.normal(key, shape, jnp.float32)
    if split:
        values = values * block_levels(key, shape, split, -0.22, 0.18)
    return jnp.clip(raised(values, jax.random.fold_in(key, 3), *heavy), -limit, limit).astype(held_as)


def setup_inputs(seed: int = 0) -> dict:
    seeds = jax.random.split(jax.random.key(seed), 14)
    layer_input = noise(seeds[0], (TOKENS, D), 1.0, 6.0, ((0, 8),))
    out_cot = bell_draw_with(seeds[1], (TOKENS, D), 1.0, 6.0, ((0, 8),), (0, 1, 8, 2.0))
    routes_keys = jax.random.split(jax.random.fold_in(seeds[2], 1), TOKENS // TOK_DEV)
    routes_turns = jax.random.permutation(jax.random.fold_in(seeds[2], 3), TOKENS // TOK_DEV)
    routes = jax.vmap(lambda own, number: routed_block(jax.random.fold_in(seeds[2], 2), own, number, TOK_DEV, EXPERTS, TOPK, CAP, 1))(routes_keys, routes_turns).reshape((TOKENS, TOPK))
    route_weights = jnp.clip(0.2 + 0.8 * jax.random.uniform(seeds[3], (TOKENS, TOPK), jnp.float32) ** block_levels(seeds[3], (TOKENS, TOPK), ((0, 8),), -0.2, 0.2), 0.2, 1.0)
    gate_weights = noise(seeds[4], (EXPERTS, D, FF), D ** -0.5, 0.125, ((0, 8), (2, 4)))
    up_weights = noise(seeds[5], (EXPERTS, D, FF), D ** -0.5, 0.125, ((0, 8), (2, 4)))
    down_weights = noise(seeds[6], (EXPERTS, FF, D), FF ** -0.5, 0.1875, ((0, 8), (1, 4)))
    out_proj = noise(seeds[7], (D, HV), HV ** -0.5, 0.125, ((1, 4),))
    queries = noise(seeds[8], (TOKENS, HV), 1.0, 6.0, ((0, 8), (1, 4)))
    keys = noise(seeds[9], (TOKENS, HV), 1.0, 6.0, ((0, 8), (1, 4)))
    values = noise(seeds[10], (TOKENS, HV), 1.0, 6.0, ((0, 8), (1, 4)))
    mixer_out = noise(seeds[11], (TOKENS, HV), 1.0, 6.0, ((0, 8), (1, 4)))
    entry_states = noise(seeds[12], (N_SP, HEADS, DK, DK), 1.0, 6.0, ((0, 8), (1, 4)), jnp.float32)
    return dict(layer_input=layer_input, out_cot=out_cot, routes=routes, route_weights=route_weights, gate_weights=gate_weights, up_weights=up_weights, down_weights=down_weights, out_proj=out_proj, queries=queries, keys=keys, values=values, mixer_out=mixer_out, entry_states=entry_states)


def decay_rates(head_ids, head_count, token_count):
    half_count = head_count // 2
    fraction = jnp.minimum(head_ids, half_count) / half_count
    base_rate = jnp.exp((1.0 - fraction) * jnp.log(1.0 / 32.0) + fraction * jnp.log(1.0 / token_count))
    return base_rate * (1.0 + jnp.maximum(head_ids - half_count, 0.0) / half_count)

def position_norm(positions, head_rates):
    return jnp.sqrt(jnp.expm1(-2.0 * head_rates)[None, :] / jnp.expm1(-2.0 * head_rates[None, :] * (positions[:, None] + 1.0)))

def rounded(values):
    return lax.optimization_barrier(values.astype(jnp.bfloat16)).astype(jnp.float32)

def retention_grads(queries, keys, values, head_cot, entry_states, head_rates):
    span_count = TOKENS // SPAN
    per_segment = TOK_DEV // SPAN
    key_scale = DK ** (-0.5)
    span_shape = (span_count, SPAN, HEADS, DK)
    query_wide = queries.reshape(span_shape).astype(jnp.float32)
    key_wide = keys.reshape(span_shape).astype(jnp.float32)
    value_wide = values.reshape(span_shape).astype(jnp.float32)
    cot_wide = head_cot.reshape(span_shape).astype(jnp.float32)
    offsets = jnp.arange(SPAN).astype(jnp.float32)
    distance = offsets[:, None] - offsets[None, :]
    decay_mat = jnp.where(distance[None] >= 0, jnp.exp(-head_rates[:, None, None] * jnp.maximum(distance, 0.0)[None]), 0.0)
    fwd_weights = rounded(jnp.einsum('cihd,cjhd->chij', query_wide, key_wide) * key_scale * decay_mat[None])
    back_weights = rounded(jnp.einsum('cihd,cjhd->chij', cot_wide, value_wide) * decay_mat[None])
    tail_decay = jnp.exp(-head_rates[None, :] * (SPAN - 1.0 - offsets)[:, None])
    lead_decay = jnp.exp(-head_rates[None, :] * (offsets + 1.0)[:, None])
    span_decay = jnp.exp(-head_rates * SPAN)
    updates = key_scale * jnp.einsum('cjhd,cjhe->chde', key_wide * tail_decay[None, :, :, None], value_wide, precision=lax.Precision.HIGHEST)
    backs = jnp.einsum('cihd,cihe->chde', query_wide * lead_decay[None, :, :, None], cot_wide, precision=lax.Precision.HIGHEST)

    def forward(carried, inputs_c):
        update, span_index = inputs_c
        saved_state = entry_states[span_index // per_segment]
        current = jnp.where(span_index % per_segment == 0, saved_state, carried)
        return (span_decay[:, None, None] * current + update, current)
    start_state = jnp.zeros((HEADS, DK, DK), jnp.float32)
    _, fwd_states = lax.scan(forward, start_state, (updates, jnp.arange(span_count, dtype=jnp.int32)))

    def backward(carried, update):
        return (span_decay[:, None, None] * carried + update, carried)
    _, rev_states = lax.scan(backward, start_state, backs, reverse=True)
    grad_q = key_scale * jnp.einsum('chij,cjhd->cihd', back_weights, key_wide)
    grad_q = grad_q + lead_decay[None, :, :, None] * jnp.einsum('chde,cihe->cihd', fwd_states, cot_wide, precision=lax.Precision.HIGHEST)
    grad_k = jnp.einsum('chij,cihd->cjhd', back_weights, query_wide)
    grad_k = key_scale * (grad_k + tail_decay[None, :, :, None] * jnp.einsum('chde,cjhe->cjhd', rev_states, value_wide, precision=lax.Precision.HIGHEST))
    grad_v = jnp.einsum('chij,cihe->cjhe', fwd_weights, cot_wide)
    grad_v = grad_v + key_scale * tail_decay[None, :, :, None] * jnp.einsum('chde,cjhd->cjhe', rev_states, key_wide, precision=lax.Precision.HIGHEST)
    flat_shape = (TOKENS, HEADS * DK)
    return (grad_q.reshape(flat_shape).astype(jnp.bfloat16), grad_k.reshape(flat_shape).astype(jnp.bfloat16), grad_v.reshape(flat_shape).astype(jnp.bfloat16))

def reference(layer_input, out_cot, routes, route_weights, gate_weights, up_weights, down_weights, out_proj, queries, keys, values, mixer_out, entry_states):
    pair_total = TOKENS * TOPK
    per_block = TOK_DEV * TOPK
    slot_count = N_SP * CAP
    flat_routes = routes.reshape(-1)
    onehot = (flat_routes.reshape(N_SP, per_block, 1) == jnp.arange(EXPERTS, dtype=jnp.int32)[None, None, :]).astype(jnp.int32)
    earlier = jnp.cumsum(onehot, axis=1) - onehot
    placed = lax.optimization_barrier(jnp.sum(earlier * onehot, axis=2)).reshape(-1)
    block_id = jnp.arange(pair_total, dtype=jnp.int32) // per_block
    target = flat_routes * slot_count + block_id * CAP + placed
    owner_tok = jnp.arange(pair_total, dtype=jnp.int32) // TOPK
    slot_tok = jnp.full((EXPERTS * slot_count,), TOKENS, jnp.int32).at[target].set(owner_tok)
    slot_weight = jnp.zeros((EXPERTS * slot_count,), jnp.float32).at[target].set(route_weights.reshape(-1))
    blank_row = jnp.zeros((1, D), jnp.bfloat16)
    input_ext = jnp.concatenate([layer_input, blank_row], 0)
    cot_ext = jnp.concatenate([out_cot, blank_row], 0)

    def expert_step(accum, inputs_e):
        gate_w, up_w, down_w, row_ids, row_weight = inputs_e
        exp_rows = input_ext[row_ids]
        exp_cot = (row_weight[:, None] * cot_ext[row_ids].astype(jnp.float32)).astype(jnp.bfloat16)
        gate_pre = jnp.dot(exp_rows, gate_w, preferred_element_type=jnp.float32)
        up_pre = jnp.dot(exp_rows, up_w, preferred_element_type=jnp.float32)
        sigmoid_g = jax.nn.sigmoid(gate_pre)
        activated = (gate_pre * sigmoid_g * up_pre).astype(jnp.bfloat16)
        grad_down = jnp.dot(activated.T, exp_cot, preferred_element_type=jnp.float32).astype(jnp.bfloat16)
        d_act = jnp.dot(exp_cot, down_w.T, preferred_element_type=jnp.float32)
        d_gate = (d_act * up_pre * sigmoid_g * (1.0 + gate_pre * (1.0 - sigmoid_g))).astype(jnp.bfloat16)
        d_up = (d_act * gate_pre * sigmoid_g).astype(jnp.bfloat16)
        grad_gate = jnp.dot(exp_rows.T, d_gate, preferred_element_type=jnp.float32).astype(jnp.bfloat16)
        grad_up = jnp.dot(exp_rows.T, d_up, preferred_element_type=jnp.float32).astype(jnp.bfloat16)
        returned = jnp.dot(d_gate, gate_w.T, preferred_element_type=jnp.float32)
        returned = returned + jnp.dot(d_up, up_w.T, preferred_element_type=jnp.float32)
        return (accum.at[row_ids].add(rounded(returned)), (grad_gate, grad_up, grad_down))
    accum, expert_out = lax.scan(expert_step, jnp.zeros((TOKENS + 1, D), jnp.float32), (gate_weights, up_weights, down_weights, slot_tok.reshape(EXPERTS, slot_count), slot_weight.reshape(EXPERTS, slot_count)))
    grad_gate, grad_up, grad_down = expert_out
    mixer_cot = (out_cot.astype(jnp.float32) + accum[:TOKENS]).astype(jnp.bfloat16)
    grad_proj = jnp.dot(mixer_cot.T, mixer_out, preferred_element_type=jnp.float32)
    head_rates = decay_rates(jnp.arange(HEADS).astype(jnp.float32), HEADS, TOKENS)
    positions = jnp.arange(TOKENS).astype(jnp.float32)
    head_cot = jnp.dot(mixer_cot, out_proj, preferred_element_type=jnp.float32).reshape(TOKENS, HEADS, DK)
    head_cot = (head_cot * position_norm(positions, head_rates)[:, :, None]).astype(jnp.bfloat16)
    grad_q, grad_k, grad_v = retention_grads(queries, keys, values, head_cot, entry_states, head_rates)
    return (grad_gate, grad_up, grad_down, grad_proj, grad_q, grad_k, grad_v)
```

```python
import functools

import jax
import jax.numpy as jnp
from jax import lax
from jax.experimental import pallas as pl
from jax.experimental.pallas import tpu as pltpu
from jax.sharding import PartitionSpec as P

DK = 64
SPAN = 128
MESH = pl.DeviceIdType.MESH
VMEM = pl.BlockSpec(memory_space=pltpu.VMEM)


def seat(experts):
    me, tp = lax.axis_index("sp"), lax.axis_index("tp")
    core, row = tp % 2, tp // 2
    return me, tp, core, row, tp + 1 - 2 * core, (tp + 2) % 4


def greet(experts, me, tp_peers):
    barrier = pltpu.get_barrier_semaphore()
    for k in range(1, experts):
        pl.semaphore_signal(
            barrier, inc=1, device_id={"sp": (me + k) % experts}, device_id_type=MESH
        )
    for peer in tp_peers:
        pl.semaphore_signal(barrier, inc=1, device_id={"tp": peer}, device_id_type=MESH)
    pl.semaphore_wait(barrier, experts - 1 + len(tp_peers))


def send(src, dst, send_sem, recv_sem, target):
    copy = pltpu.make_async_remote_copy(
        src_ref=src,
        dst_ref=dst,
        send_sem=send_sem,
        recv_sem=recv_sem,
        device_id=target,
        device_id_type=MESH,
    )
    copy.start()
    return copy


def dispatch_kernel(
    experts, rows, cot, out_rows, out_cot, own, s_sp, r_sp, s_y, r_y, s_c, r_c
):
    me, tp, core, row, mate, across = seat(experts)
    greet(experts, me, (mate, across))
    arrays = ((rows, out_rows), (cot, out_cot))
    far = {}
    for k in range(1, experts):
        peer = (me + k) % experts
        for a, (src, dst) in enumerate(arrays):
            far[a, k] = send(
                src.at[peer], dst.at[me, tp], s_sp.at[a, k], r_sp.at[a, k], {"sp": peer}
            )
    local = []
    for a, (src, dst) in enumerate(arrays):
        copy = pltpu.make_async_copy(src.at[me], dst.at[me, tp], own.at[a])
        copy.start()
        local.append(copy)
    for copy in local:
        copy.wait()
    side, near, relayed = {}, {}, {}

    def relay(k):
        origin = (me - k + experts) % experts
        for a, (src, dst) in enumerate(arrays):
            side[a, k].wait_recv()
            held = dst.at[origin, across]
            relayed[a, k] = send(held, held, s_c.at[a, 1, k], r_c.at[a, 1, k], {"tp": mate})

    for k in range(experts):
        origin = (me - k + experts) % experts
        for a, (src, dst) in enumerate(arrays):
            if k > 0:
                far[a, k].wait_recv()
            held = dst.at[origin, tp]
            side[a, k] = send(held, held, s_y.at[a, k], r_y.at[a, k], {"tp": across})
            near[a, k] = send(held, held, s_c.at[a, 0, k], r_c.at[a, 0, k], {"tp": mate})
        if k > 1:
            relay(k - 2)
    relay(experts - 2)
    relay(experts - 1)
    for copy in list(near.values()) + list(relayed.values()):
        copy.wait_recv()
    for group in (far, side, near, relayed):
        for copy in group.values():
            copy.wait_send()


def dispatch(rows, cot, narrow):
    experts, share, width = rows.shape
    full = jax.ShapeDtypeStruct((experts, narrow, share, width), rows.dtype)
    sem = pltpu.SemaphoreType.DMA
    return pl.pallas_call(
        functools.partial(dispatch_kernel, experts),
        out_shape=(full, full),
        in_specs=[VMEM, VMEM],
        out_specs=(VMEM, VMEM),
        scratch_shapes=[
            sem((2,)),
            sem((2, experts)),
            sem((2, experts)),
            sem((2, experts)),
            sem((2, experts)),
            sem((2, 2, experts)),
            sem((2, 2, experts)),
        ],
        compiler_params=pltpu.CompilerParams(collective_id=0, has_side_effects=True),
    )(rows, cot)


def combine_kernel(
    experts,
    part,
    picks,
    own_cot,
    mixer,
    near_buf,
    side_out,
    side_in,
    far_out,
    back,
    s_c,
    r_c,
    s_y,
    r_y,
    s_f,
    r_f,
    s_g,
    r_g,
):
    me, tp, core, row, mate, across = seat(experts)
    cols = part.shape[2] // 4

    def quarter(index):
        return pl.ds(pl.multiple_of(index * cols, cols), cols)

    greet(experts, me, (mate, across))
    order = list(range(1, experts)) + [0]
    near, side, far = {}, {}, {}
    mate_core = 1 - core
    for k in order:
        dest = (me + k) % experts
        for half in range(2):
            near[k, half] = send(
                part.at[dest, :, quarter(half * 2 + mate_core)],
                near_buf.at[k, half],
                s_c.at[k, half],
                r_c.at[k, half],
                {"tp": mate},
            )
    for k in order:
        dest = (me + k) % experts
        near[k, 0].wait_recv()
        near[k, 1].wait_recv()
        side_out[k] = (
            part[dest, :, quarter(across)].astype(jnp.float32)
            + near_buf[k, 1 - row].astype(jnp.float32)
        ).astype(jnp.bfloat16)
        side[k] = send(side_out.at[k], side_in.at[k], s_y.at[k], r_y.at[k], {"tp": across})
    for k in order:
        dest = (me + k) % experts
        side[k].wait_recv()
        done = (
            part[dest, :, quarter(tp)].astype(jnp.float32)
            + near_buf[k, row].astype(jnp.float32)
            + side_in[k].astype(jnp.float32)
        ).astype(jnp.bfloat16)
        if k == 0:
            back[me] = done
        else:
            far_out[k] = done
            far[k] = send(far_out.at[k], back.at[me], s_f.at[k], r_f.at[k], {"sp": dest})
    for k in range(1, experts):
        far[k].wait_recv()
    slots = back[...].reshape(experts * part.shape[1], cols)
    total = own_cot[:, quarter(tp)].astype(jnp.float32) + jnp.dot(
        picks[...], slots, preferred_element_type=jnp.float32
    )
    mixer[:, quarter(tp)] = total.astype(jnp.bfloat16)
    mine = mixer.at[:, quarter(tp)]
    other = mixer.at[:, quarter(across)]
    last = [
        send(mine, mine, s_g.at[0], r_g.at[0], {"tp": across}),
        send(mine, mine, s_g.at[1], r_g.at[1], {"tp": mate}),
    ]
    last[0].wait_recv()
    last.append(send(other, other, s_g.at[2], r_g.at[2], {"tp": mate}))
    last[1].wait_recv()
    last[2].wait_recv()
    for group in (near.values(), side.values(), far.values(), last):
        for copy in group:
            copy.wait_send()


def combine(part, picks, own_cot):
    experts, capacity, width = part.shape
    tok_rows = own_cot.shape[0]
    cols = width // 4
    sem = pltpu.SemaphoreType.DMA
    block = pltpu.VMEM((experts, capacity, cols), jnp.bfloat16)
    return pl.pallas_call(
        functools.partial(combine_kernel, experts),
        out_shape=jax.ShapeDtypeStruct((tok_rows, width), jnp.bfloat16),
        in_specs=[VMEM, VMEM, VMEM],
        out_specs=VMEM,
        scratch_shapes=[
            pltpu.VMEM((experts, 2, capacity, cols), jnp.bfloat16),
            block,
            block,
            block,
            block,
            sem((experts, 2)),
            sem((experts, 2)),
            sem((experts,)),
            sem((experts,)),
            sem((experts,)),
            sem((experts,)),
            sem((3,)),
            sem((3,)),
        ],
        compiler_params=pltpu.CompilerParams(collective_id=1, has_side_effects=True),
    )(part, picks, own_cot)


def spread_kernel(experts, mixer, state, all_mixer, all_state, own, s_m, r_m, s_s, r_s):
    me = lax.axis_index("sp")
    cols = mixer.shape[1] // experts
    greet(experts, me, ())

    def block(index):
        return mixer.at[:, pl.ds(pl.multiple_of(index * cols, cols), cols)]

    copies = []
    for k in range(1, experts):
        peer = (me + k) % experts
        copies.append(send(state, all_state.at[me], s_s.at[k], r_s.at[k], {"sp": peer}))
    for k in range(1, experts):
        peer = (me + k) % experts
        copies.append(
            send(block(peer), all_mixer.at[me], s_m.at[k], r_m.at[k], {"sp": peer})
        )
    local = [
        pltpu.make_async_copy(state, all_state.at[me], own.at[0]),
        pltpu.make_async_copy(block(me), all_mixer.at[me], own.at[1]),
    ]
    for copy in local:
        copy.start()
    for copy in local:
        copy.wait()
    for copy in copies:
        copy.wait_recv()
    for copy in copies:
        copy.wait_send()


def spread(mixer, state, experts):
    sem = pltpu.SemaphoreType.DMA
    tok_rows, width = mixer.shape
    return pl.pallas_call(
        functools.partial(spread_kernel, experts),
        out_shape=(
            jax.ShapeDtypeStruct((experts, tok_rows, width // experts), mixer.dtype),
            jax.ShapeDtypeStruct((experts,) + state.shape, state.dtype),
        ),
        in_specs=[VMEM, VMEM],
        out_specs=(VMEM, VMEM),
        scratch_shapes=[
            sem((2,)),
            sem((experts,)),
            sem((experts,)),
            sem((experts,)),
            sem((experts,)),
        ],
        compiler_params=pltpu.CompilerParams(collective_id=2, has_side_effects=True),
    )(mixer, state)


def decay_rates(head_ids, head_count, token_count):
    half_count = head_count // 2
    fraction = jnp.minimum(head_ids, half_count) / half_count
    base_rate = jnp.exp(
        (1.0 - fraction) * jnp.log(1.0 / 32.0) + fraction * jnp.log(1.0 / token_count)
    )
    return base_rate * (1.0 + jnp.maximum(head_ids - half_count, 0.0) / half_count)


def position_norm(positions, head_rates):
    return jnp.sqrt(
        jnp.expm1(-2.0 * head_rates)[None, :]
        / jnp.expm1(-2.0 * head_rates[None, :] * (positions[:, None] + 1.0))
    )


def expert_grads(exp_rows, exp_cot, activated, d_gate, d_up):
    row_dims = (((0,), (0,)), ((), ()))
    grad_gate = lax.dot_general(
        exp_rows, d_gate, row_dims, preferred_element_type=jnp.float32
    ).astype(jnp.bfloat16)
    grad_up = lax.dot_general(exp_rows, d_up, row_dims, preferred_element_type=jnp.float32).astype(
        jnp.bfloat16
    )
    grad_down = lax.dot_general(
        activated, exp_cot, row_dims, preferred_element_type=jnp.float32
    ).astype(jnp.bfloat16)
    return (grad_gate[None], grad_up[None], grad_down[None])


def per_device(
    layer_input,
    out_cot,
    routes,
    route_weights,
    gate_weights,
    up_weights,
    down_weights,
    out_proj,
    queries,
    keys,
    values,
    mixer_out,
    entry_states,
):
    tok_rows, model_width = layer_input.shape
    experts = lax.axis_size("sp")
    narrow = lax.axis_size("tp")
    top_count = routes.shape[1]
    pair_count = tok_rows * top_count
    capacity = 2 * pair_count // experts
    flat_routes = routes.reshape(pair_count)
    onehot = (flat_routes[:, None] == jnp.arange(experts, dtype=jnp.int32)[None, :]).astype(
        jnp.int32
    )
    earlier = jnp.cumsum(onehot, axis=0) - onehot
    target = flat_routes * capacity + jnp.sum(earlier * onehot, axis=1)
    share = capacity // narrow
    first_row = lax.axis_index("tp") * share
    fused = narrow == 4 and share % 16 == 0 and model_width % (experts * 128) == 0
    if fused:
        pair_slot = target.reshape(tok_rows, top_count)
        part_slot = (
            jnp.arange(experts, dtype=jnp.int32)[:, None] * capacity
            + first_row
            + jnp.arange(share, dtype=jnp.int32)[None, :]
        ).reshape(experts * share)
        hits = part_slot[:, None, None] == pair_slot[None]
        part_weight = jnp.sum(jnp.where(hits, route_weights[None], 0.0), axis=(1, 2))
        chosen = jnp.any(hits, axis=2).astype(jnp.bfloat16)
        part_rows = jnp.dot(chosen, layer_input, preferred_element_type=jnp.float32)
        part_cot = jnp.dot(chosen, out_cot, preferred_element_type=jnp.float32)
        part_shape = (experts, share, model_width)
        got_rows, got_cot = dispatch(
            part_rows.astype(jnp.bfloat16).reshape(part_shape),
            (part_weight[:, None] * part_cot).astype(jnp.bfloat16).reshape(part_shape),
            narrow,
        )
        all_slots = jnp.arange(experts * capacity, dtype=jnp.int32)
        picks = jnp.any(pair_slot[:, :, None] == all_slots[None, None], axis=1).astype(
            jnp.bfloat16
        )
    else:
        owner_tok = jnp.arange(pair_count, dtype=jnp.int32) // top_count
        slot_tok = jnp.full((experts * capacity,), tok_rows, jnp.int32).at[target].set(owner_tok)
        slot_weight = (
            jnp.zeros((experts * capacity,), jnp.float32)
            .at[target]
            .set(route_weights.reshape(pair_count))
        )
        blank_row = jnp.zeros((1, model_width), jnp.bfloat16)
        sent_rows = jnp.concatenate([layer_input, blank_row], 0)[slot_tok].reshape(
            experts, capacity, model_width
        )
        picked_cot = jnp.concatenate([out_cot, blank_row], 0)[slot_tok]
        sent_cot = (
            (slot_weight[:, None] * picked_cot.astype(jnp.float32))
            .astype(jnp.bfloat16)
            .reshape(experts, capacity, model_width)
        )
        part_rows = lax.dynamic_slice_in_dim(sent_rows, first_row, share, 1)
        part_cot = lax.dynamic_slice_in_dim(sent_cot, first_row, share, 1)
        got_rows, got_cot = (
            lax.all_to_all(part_rows, "sp", split_axis=0, concat_axis=0, tiled=True),
            lax.all_to_all(part_cot, "sp", split_axis=0, concat_axis=0, tiled=True),
        )
        got_rows, got_cot = (
            lax.all_gather(got_rows, "tp", axis=1, tiled=True),
            lax.all_gather(got_cot, "tp", axis=1, tiled=True),
        )
    exp_rows = got_rows.reshape(experts * capacity, model_width)
    exp_cot = got_cot.reshape(experts * capacity, model_width)
    gate_w = gate_weights[0]
    up_w = up_weights[0]
    down_w = down_weights[0]
    gate_pre = jnp.dot(exp_rows, gate_w, preferred_element_type=jnp.float32)
    up_pre = jnp.dot(exp_rows, up_w, preferred_element_type=jnp.float32)
    sigmoid_g = jax.nn.sigmoid(gate_pre)
    activated = (gate_pre * sigmoid_g * up_pre).astype(jnp.bfloat16)
    width_dims = (((1,), (1,)), ((), ()))
    d_act = lax.dot_general(exp_cot, down_w, width_dims, preferred_element_type=jnp.float32)
    d_gate = (d_act * up_pre * sigmoid_g * (1.0 + gate_pre * (1.0 - sigmoid_g))).astype(
        jnp.bfloat16
    )
    d_up = (d_act * gate_pre * sigmoid_g).astype(jnp.bfloat16)
    grads = expert_grads(exp_rows, exp_cot, activated, d_gate, d_up)
    partial_sum = lax.dot_general(d_gate, gate_w, width_dims, preferred_element_type=jnp.float32)
    partial_sum = partial_sum + lax.dot_general(
        d_up, up_w, width_dims, preferred_element_type=jnp.float32
    )
    if fused:
        mixer_cot = combine(
            partial_sum.astype(jnp.bfloat16).reshape(experts, capacity, model_width),
            picks,
            out_cot,
        )
    else:
        summed = lax.psum_scatter(
            partial_sum.reshape(experts, capacity, model_width), "tp", scatter_dimension=2, tiled=True
        )
        returned = lax.all_to_all(
            summed.astype(jnp.bfloat16), "sp", split_axis=0, concat_axis=0, tiled=True
        )
        col_count = model_width // narrow
        first_col = lax.axis_index("tp") * col_count
        back_flat = returned.reshape(experts * capacity, col_count)
        pair_back = back_flat[target].reshape(tok_rows, top_count, col_count).astype(jnp.float32)
        own_cols = lax.dynamic_slice_in_dim(out_cot, first_col, col_count, 1).astype(jnp.float32)
        cot_cols = (own_cols + jnp.sum(pair_back, axis=1)).astype(jnp.bfloat16)
        mixer_cot = lax.all_gather(cot_cols, "tp", axis=1, tiled=True)
    head_count = queries.shape[1] // DK
    head_ids = (lax.axis_index("tp") * head_count + jnp.arange(head_count, dtype=jnp.int32)).astype(
        jnp.float32
    )
    head_rates = decay_rates(head_ids, head_count * narrow, tok_rows * experts)
    positions = (lax.axis_index("sp") * tok_rows + jnp.arange(tok_rows, dtype=jnp.int32)).astype(
        jnp.float32
    )
    head_cot = jnp.dot(mixer_cot, out_proj, preferred_element_type=jnp.float32).reshape(
        tok_rows, head_count, DK
    )
    head_cot = (head_cot * position_norm(positions, head_rates)[:, :, None]).astype(jnp.bfloat16)
    span_count = tok_rows // SPAN
    span_shape = (span_count, SPAN, head_count, DK)
    span_query = queries.reshape(span_shape)
    span_key = keys.reshape(span_shape)
    span_value = values.reshape(span_shape)
    span_cot = head_cot.reshape(span_shape)
    key_scale = DK ** (-0.5)
    offsets = jnp.arange(SPAN, dtype=jnp.float32)
    distance = offsets[:, None] - offsets[None, :]
    decay_mat = jnp.where(
        distance[None] >= 0,
        jnp.exp(-head_rates[:, None, None] * jnp.maximum(distance, 0.0)[None]),
        0.0,
    )
    fwd_weights = (
        jnp.einsum("cihd,cjhd->chij", span_query, span_key, preferred_element_type=jnp.float32)
        * key_scale
        * decay_mat[None]
    ).astype(jnp.bfloat16)
    back_weights = (
        jnp.einsum("cihd,cjhd->chij", span_cot, span_value, preferred_element_type=jnp.float32)
        * decay_mat[None]
    ).astype(jnp.bfloat16)
    tail_decay = jnp.exp(-head_rates[None, :] * (SPAN - 1.0 - offsets)[:, None])
    lead_decay = jnp.exp(-head_rates[None, :] * (offsets + 1.0)[:, None])
    query_wide = span_query.astype(jnp.float32)
    key_wide = span_key.astype(jnp.float32)
    value_wide = span_value.astype(jnp.float32)
    cot_wide = span_cot.astype(jnp.float32)
    backs = jnp.einsum(
        "cihd,cihe->chde",
        query_wide * lead_decay[None, :, :, None],
        cot_wide,
        precision=lax.Precision.HIGHEST,
    )
    own_back = backs[0]
    if fused:
        packed = own_back.astype(jnp.bfloat16).reshape(head_count * DK // 2, 2 * DK)
        all_mixer, all_backs = spread(mixer_cot, packed, experts)
        all_backs = all_backs.reshape((experts,) + own_back.shape).astype(jnp.float32)
        all_out = jnp.concatenate(
            [mixer_out]
            + [
                lax.ppermute(mixer_out, "sp", [(i, (i + k) % experts) for i in range(experts)])
                for k in range(1, experts)
            ],
            axis=0,
        )
        device = lax.axis_index("sp")
        sources = (device - jnp.arange(experts)) % experts
        all_mixer = all_mixer[sources]
        grad_proj = lax.dot_general(
            all_mixer.reshape(experts * tok_rows, model_width // experts),
            all_out,
            (((0,), (0,)), ((), ())),
            preferred_element_type=jnp.float32,
        )
    else:
        all_backs = lax.all_gather(own_back, "sp")
        grad_proj = lax.psum_scatter(
            lax.dot_general(
                mixer_cot, mixer_out, (((0,), (0,)), ((), ())), preferred_element_type=jnp.float32
            ),
            "sp",
            scatter_dimension=0,
            tiled=True,
        )
    ahead = jnp.arange(experts, dtype=jnp.int32) - lax.axis_index("sp") - 1
    reach = jnp.where(
        ahead[:, None] >= 0,
        jnp.exp(-head_rates[None, :] * (jnp.maximum(ahead, 0) * tok_rows)[:, None]),
        0.0,
    )
    rev_states = jnp.sum(reach[:, :, None, None] * all_backs, axis=0)[None]
    fwd_stack = entry_states
    grad_q = key_scale * jnp.einsum(
        "chij,cjhd->cihd", back_weights, span_key, preferred_element_type=jnp.float32
    )
    grad_q = grad_q + lead_decay[None, :, :, None] * jnp.einsum(
        "chde,cihe->cihd", fwd_stack, cot_wide, precision=lax.Precision.HIGHEST
    )
    grad_k = jnp.einsum(
        "chij,cihd->cjhd", back_weights, span_query, preferred_element_type=jnp.float32
    )
    grad_k = key_scale * (
        grad_k
        + tail_decay[None, :, :, None]
        * jnp.einsum("chde,cjhe->cjhd", rev_states, value_wide, precision=lax.Precision.HIGHEST)
    )
    grad_v = jnp.einsum(
        "chij,cihe->cjhe", fwd_weights, span_cot, preferred_element_type=jnp.float32
    )
    grad_v = grad_v + key_scale * tail_decay[None, :, :, None] * jnp.einsum(
        "chde,cjhd->cjhe", rev_states, key_wide, precision=lax.Precision.HIGHEST
    )
    flat_shape = (tok_rows, head_count * DK)
    return (
        grads[0],
        grads[1],
        grads[2],
        grad_proj,
        grad_q.reshape(flat_shape).astype(jnp.bfloat16),
        grad_k.reshape(flat_shape).astype(jnp.bfloat16),
        grad_v.reshape(flat_shape).astype(jnp.bfloat16),
    )


def solution(mesh):
    placed = (
        P("sp", None),
        P("sp", None),
        P("sp", None),
        P("sp", None),
        P("sp", None, "tp"),
        P("sp", None, "tp"),
        P("sp", "tp", None),
        P(None, "tp"),
        P("sp", "tp"),
        P("sp", "tp"),
        P("sp", "tp"),
        P("sp", "tp"),
        P("sp", "tp", None, None),
    )
    return jax.shard_map(
        per_device,
        mesh=mesh,
        in_specs=placed,
        out_specs=(
            P("sp", None, "tp"),
            P("sp", None, "tp"),
            P("sp", "tp", None),
            P("sp", "tp"),
            P("sp", "tp"),
            P("sp", "tp"),
            P("sp", "tp"),
        ),
        check_vma=False,
    )
```

```python
import functools

import jax
import jax.numpy as jnp
from jax import lax
from jax.experimental import pallas as pl
from jax.experimental.pallas import tpu as pltpu
from jax.sharding import PartitionSpec as P

DK = 64
SPAN = 128
MESH = pl.DeviceIdType.MESH
VMEM = pl.BlockSpec(memory_space=pltpu.VMEM)


def seat(experts):
    me, tp = lax.axis_index("sp"), lax.axis_index("tp")
    core, row = tp % 2, tp // 2
    return me, tp, core, row, tp + 1 - 2 * core, (tp + 2) % 4


def greet(experts, me, tp_peers):
    barrier = pltpu.get_barrier_semaphore()
    for k in range(1, experts):
        pl.semaphore_signal(
            barrier, inc=1, device_id={"sp": (me + k) % experts}, device_id_type=MESH
        )
    for peer in tp_peers:
        pl.semaphore_signal(barrier, inc=1, device_id={"tp": peer}, device_id_type=MESH)
    pl.semaphore_wait(barrier, experts - 1 + len(tp_peers))


def send(src, dst, send_sem, recv_sem, target):
    copy = pltpu.make_async_remote_copy(
        src_ref=src,
        dst_ref=dst,
        send_sem=send_sem,
        recv_sem=recv_sem,
        device_id=target,
        device_id_type=MESH,
    )
    copy.start()
    return copy


def share_rows(experts, me, src, whole, own, s_r, r_r):
    mate = me + 1 - 2 * (me % 2)
    hops = []
    for k in range(1, experts // 2):
        peer = (me + 2 * k) % experts
        hops.append(send(src, whole.at[me], s_r.at[0, k], r_r.at[0, k], {"sp": peer}))
    relays = [send(src, whole.at[me], s_r.at[1, 0], r_r.at[1, 0], {"sp": mate})]
    local = pltpu.make_async_copy(src, whole.at[me], own)
    local.start()

    def relay():
        for k in range(1, experts // 2):
            hops[k - 1].wait_recv()
            held = whole.at[(me - 2 * k + experts) % experts]
            relays.append(send(held, held, s_r.at[1, k], r_r.at[1, k], {"sp": mate}))

    def arrive():
        local.wait()
        for copy in relays:
            copy.wait_recv()

    def drain():
        for copy in hops + relays:
            copy.wait_send()

    return relay, arrive, drain


def dispatch_kernel(
    experts, rows, cot, out_rows, out_cot, own, s_sp, r_sp, s_y, r_y, s_c, r_c
):
    me, tp, core, row, mate, across = seat(experts)
    greet(experts, me, (mate, across))
    arrays = ((rows, out_rows), (cot, out_cot))
    far = {}
    for k in range(1, experts):
        peer = (me + k) % experts
        for a, (src, dst) in enumerate(arrays):
            far[a, k] = send(
                src.at[peer], dst.at[me, tp], s_sp.at[a, k], r_sp.at[a, k], {"sp": peer}
            )
    local = []
    for a, (src, dst) in enumerate(arrays):
        copy = pltpu.make_async_copy(src.at[me], dst.at[me, tp], own.at[a])
        copy.start()
        local.append(copy)
    for copy in local:
        copy.wait()
    side, near, relayed = {}, {}, {}

    def relay(k):
        origin = (me - k + experts) % experts
        for a, (src, dst) in enumerate(arrays):
            side[a, k].wait_recv()
            held = dst.at[origin, across]
            relayed[a, k] = send(held, held, s_c.at[a, 1, k], r_c.at[a, 1, k], {"tp": mate})

    for k in range(experts):
        origin = (me - k + experts) % experts
        for a, (src, dst) in enumerate(arrays):
            if k > 0:
                far[a, k].wait_recv()
            held = dst.at[origin, tp]
            side[a, k] = send(held, held, s_y.at[a, k], r_y.at[a, k], {"tp": across})
            near[a, k] = send(held, held, s_c.at[a, 0, k], r_c.at[a, 0, k], {"tp": mate})
        if k > 1:
            relay(k - 2)
    relay(experts - 2)
    relay(experts - 1)
    for copy in list(near.values()) + list(relayed.values()):
        copy.wait_recv()
    for group in (far, side, near, relayed):
        for copy in group.values():
            copy.wait_send()


def dispatch(rows, cot, narrow):
    experts, share, width = rows.shape
    full = jax.ShapeDtypeStruct((experts, narrow, share, width), rows.dtype)
    sem = pltpu.SemaphoreType.DMA
    return pl.pallas_call(
        functools.partial(dispatch_kernel, experts),
        out_shape=(full, full),
        in_specs=[VMEM, VMEM],
        out_specs=(VMEM, VMEM),
        scratch_shapes=[
            sem((2,)),
            sem((2, experts)),
            sem((2, experts)),
            sem((2, experts)),
            sem((2, experts)),
            sem((2, 2, experts)),
            sem((2, 2, experts)),
        ],
        compiler_params=pltpu.CompilerParams(collective_id=0, has_side_effects=True),
    )(rows, cot)


def combine_kernel(
    experts,
    part,
    picks,
    own_cot,
    out_rows,
    mixer,
    all_out,
    near_buf,
    side_out,
    side_in,
    far_out,
    back,
    s_c,
    r_c,
    s_y,
    r_y,
    s_f,
    r_f,
    s_g,
    r_g,
    own,
    s_r,
    r_r,
):
    me, tp, core, row, mate, across = seat(experts)
    cols = part.shape[2] // 4

    def quarter(index):
        return pl.ds(pl.multiple_of(index * cols, cols), cols)

    greet(experts, me, (mate, across))
    order = list(range(1, experts)) + [0]
    relay, arrive, drain = share_rows(experts, me, out_rows, all_out, own.at[0], s_r, r_r)
    near, side, far = {}, {}, {}
    mate_core = 1 - core
    for k in order:
        dest = (me + k) % experts
        for half in range(2):
            near[k, half] = send(
                part.at[dest, :, quarter(half * 2 + mate_core)],
                near_buf.at[k, half],
                s_c.at[k, half],
                r_c.at[k, half],
                {"tp": mate},
            )
    for k in order:
        dest = (me + k) % experts
        near[k, 0].wait_recv()
        near[k, 1].wait_recv()
        side_out[k] = (
            part[dest, :, quarter(across)].astype(jnp.float32)
            + near_buf[k, 1 - row].astype(jnp.float32)
        ).astype(jnp.bfloat16)
        side[k] = send(side_out.at[k], side_in.at[k], s_y.at[k], r_y.at[k], {"tp": across})
    for k in order:
        dest = (me + k) % experts
        side[k].wait_recv()
        done = (
            part[dest, :, quarter(tp)].astype(jnp.float32)
            + near_buf[k, row].astype(jnp.float32)
            + side_in[k].astype(jnp.float32)
        ).astype(jnp.bfloat16)
        if k == 0:
            back[me] = done
        else:
            far_out[k] = done
            far[k] = send(far_out.at[k], back.at[me], s_f.at[k], r_f.at[k], {"sp": dest})
    relay()
    for k in range(1, experts):
        far[k].wait_recv()
    slots = back[...].reshape(experts * part.shape[1], cols)
    total = own_cot[:, quarter(tp)].astype(jnp.float32) + jnp.dot(
        picks[...], slots, preferred_element_type=jnp.float32
    )
    mixer[:, quarter(tp)] = total.astype(jnp.bfloat16)
    mine = mixer.at[:, quarter(tp)]
    other = mixer.at[:, quarter(across)]
    last = [
        send(mine, mine, s_g.at[0], r_g.at[0], {"tp": across}),
        send(mine, mine, s_g.at[1], r_g.at[1], {"tp": mate}),
    ]
    last[0].wait_recv()
    last.append(send(other, other, s_g.at[2], r_g.at[2], {"tp": mate}))
    last[1].wait_recv()
    last[2].wait_recv()
    arrive()
    drain()
    for group in (near.values(), side.values(), far.values(), last):
        for copy in group:
            copy.wait_send()


def combine(part, picks, own_cot, out_rows):
    experts, capacity, width = part.shape
    tok_rows = own_cot.shape[0]
    cols = width // 4
    sem = pltpu.SemaphoreType.DMA
    block = pltpu.VMEM((experts, capacity, cols), jnp.bfloat16)
    return pl.pallas_call(
        functools.partial(combine_kernel, experts),
        out_shape=(
            jax.ShapeDtypeStruct((tok_rows, width), jnp.bfloat16),
            jax.ShapeDtypeStruct((experts,) + out_rows.shape, out_rows.dtype),
        ),
        in_specs=[VMEM, VMEM, VMEM, VMEM],
        out_specs=(VMEM, VMEM),
        scratch_shapes=[
            pltpu.VMEM((experts, 2, capacity, cols), jnp.bfloat16),
            block,
            block,
            block,
            block,
            sem((experts, 2)),
            sem((experts, 2)),
            sem((experts,)),
            sem((experts,)),
            sem((experts,)),
            sem((experts,)),
            sem((3,)),
            sem((3,)),
            sem((1,)),
            sem((2, experts // 2)),
            sem((2, experts // 2)),
        ],
        compiler_params=pltpu.CompilerParams(collective_id=1, has_side_effects=True),
    )(part, picks, own_cot, out_rows)


def spread_kernel(
    experts, mixer, state, reach, all_mixer, later, all_state, own, s_m, r_m, s_r, r_r
):
    me = lax.axis_index("sp")
    cols = mixer.shape[1] // experts
    greet(experts, me, ())

    def block(index):
        return mixer.at[:, pl.ds(pl.multiple_of(index * cols, cols), cols)]

    relay, arrive, drain = share_rows(experts, me, state, all_state, own.at[0], s_r, r_r)
    copies = []
    for k in range(1, experts):
        peer = (me + k) % experts
        copies.append(
            send(block(peer), all_mixer.at[me], s_m.at[k], r_m.at[k], {"sp": peer})
        )
    local = pltpu.make_async_copy(block(me), all_mixer.at[me], own.at[1])
    local.start()
    relay()
    local.wait()
    arrive()
    total = jnp.zeros(later.shape, jnp.float32)
    for j in range(experts):
        total = total + reach[:, j : j + 1] * all_state[j].astype(jnp.float32)
    later[...] = total
    for copy in copies:
        copy.wait_recv()
    for copy in copies:
        copy.wait_send()
    drain()


def spread(mixer, state, reach):
    sem = pltpu.SemaphoreType.DMA
    tok_rows, width = mixer.shape
    experts = reach.shape[1]
    return pl.pallas_call(
        functools.partial(spread_kernel, experts),
        out_shape=(
            jax.ShapeDtypeStruct((experts, tok_rows, width // experts), mixer.dtype),
            jax.ShapeDtypeStruct(state.shape, jnp.float32),
        ),
        in_specs=[VMEM, VMEM, VMEM],
        out_specs=(VMEM, VMEM),
        scratch_shapes=[
            pltpu.VMEM((experts,) + state.shape, state.dtype),
            sem((2,)),
            sem((experts,)),
            sem((experts,)),
            sem((2, experts // 2)),
            sem((2, experts // 2)),
        ],
        compiler_params=pltpu.CompilerParams(collective_id=2, has_side_effects=True),
    )(mixer, state, reach)


def decay_rates(head_ids, head_count, token_count):
    half_count = head_count // 2
    fraction = jnp.minimum(head_ids, half_count) / half_count
    base_rate = jnp.exp(
        (1.0 - fraction) * jnp.log(1.0 / 32.0) + fraction * jnp.log(1.0 / token_count)
    )
    return base_rate * (1.0 + jnp.maximum(head_ids - half_count, 0.0) / half_count)


def position_norm(positions, head_rates):
    return jnp.sqrt(
        jnp.expm1(-2.0 * head_rates)[None, :]
        / jnp.expm1(-2.0 * head_rates[None, :] * (positions[:, None] + 1.0))
    )


def expert_grads(exp_rows, exp_cot, activated, d_gate, d_up):
    row_dims = (((0,), (0,)), ((), ()))
    grad_gate = lax.dot_general(
        exp_rows, d_gate, row_dims, preferred_element_type=jnp.float32
    ).astype(jnp.bfloat16)
    grad_up = lax.dot_general(exp_rows, d_up, row_dims, preferred_element_type=jnp.float32).astype(
        jnp.bfloat16
    )
    grad_down = lax.dot_general(
        activated, exp_cot, row_dims, preferred_element_type=jnp.float32
    ).astype(jnp.bfloat16)
    return (grad_gate[None], grad_up[None], grad_down[None])


def per_device(
    layer_input,
    out_cot,
    routes,
    route_weights,
    gate_weights,
    up_weights,
    down_weights,
    out_proj,
    queries,
    keys,
    values,
    mixer_out,
    entry_states,
):
    tok_rows, model_width = layer_input.shape
    experts = lax.axis_size("sp")
    narrow = lax.axis_size("tp")
    top_count = routes.shape[1]
    pair_count = tok_rows * top_count
    capacity = 2 * pair_count // experts
    flat_routes = routes.reshape(pair_count)
    onehot = (flat_routes[:, None] == jnp.arange(experts, dtype=jnp.int32)[None, :]).astype(
        jnp.int32
    )
    earlier = jnp.cumsum(onehot, axis=0) - onehot
    target = flat_routes * capacity + jnp.sum(earlier * onehot, axis=1)
    share = capacity // narrow
    first_row = lax.axis_index("tp") * share
    fused = narrow == 4 and experts % 2 == 0 and share % 16 == 0 and model_width % (experts * 128) == 0
    if fused:
        pair_slot = target.reshape(tok_rows, top_count)
        part_slot = (
            jnp.arange(experts, dtype=jnp.int32)[:, None] * capacity
            + first_row
            + jnp.arange(share, dtype=jnp.int32)[None, :]
        ).reshape(experts * share)
        hits = part_slot[:, None, None] == pair_slot[None]
        part_weight = jnp.sum(jnp.where(hits, route_weights[None], 0.0), axis=(1, 2))
        chosen = jnp.any(hits, axis=2).astype(jnp.bfloat16)
        part_rows = jnp.dot(chosen, layer_input, preferred_element_type=jnp.float32)
        part_cot = jnp.dot(chosen, out_cot, preferred_element_type=jnp.float32)
        part_shape = (experts, share, model_width)
        got_rows, got_cot = dispatch(
            part_rows.astype(jnp.bfloat16).reshape(part_shape),
            (part_weight[:, None] * part_cot).astype(jnp.bfloat16).reshape(part_shape),
            narrow,
        )
        all_slots = jnp.arange(experts * capacity, dtype=jnp.int32)
        picks = jnp.any(pair_slot[:, :, None] == all_slots[None, None], axis=1).astype(
            jnp.bfloat16
        )
    else:
        owner_tok = jnp.arange(pair_count, dtype=jnp.int32) // top_count
        slot_tok = jnp.full((experts * capacity,), tok_rows, jnp.int32).at[target].set(owner_tok)
        slot_weight = (
            jnp.zeros((experts * capacity,), jnp.float32)
            .at[target]
            .set(route_weights.reshape(pair_count))
        )
        blank_row = jnp.zeros((1, model_width), jnp.bfloat16)
        sent_rows = jnp.concatenate([layer_input, blank_row], 0)[slot_tok].reshape(
            experts, capacity, model_width
        )
        picked_cot = jnp.concatenate([out_cot, blank_row], 0)[slot_tok]
        sent_cot = (
            (slot_weight[:, None] * picked_cot.astype(jnp.float32))
            .astype(jnp.bfloat16)
            .reshape(experts, capacity, model_width)
        )
        part_rows = lax.dynamic_slice_in_dim(sent_rows, first_row, share, 1)
        part_cot = lax.dynamic_slice_in_dim(sent_cot, first_row, share, 1)
        got_rows, got_cot = (
            lax.all_to_all(part_rows, "sp", split_axis=0, concat_axis=0, tiled=True),
            lax.all_to_all(part_cot, "sp", split_axis=0, concat_axis=0, tiled=True),
        )
        got_rows, got_cot = (
            lax.all_gather(got_rows, "tp", axis=1, tiled=True),
            lax.all_gather(got_cot, "tp", axis=1, tiled=True),
        )
    exp_rows = got_rows.reshape(experts * capacity, model_width)
    exp_cot = got_cot.reshape(experts * capacity, model_width)
    gate_w = gate_weights[0]
    up_w = up_weights[0]
    down_w = down_weights[0]
    gate_pre = jnp.dot(exp_rows, gate_w, preferred_element_type=jnp.float32)
    up_pre = jnp.dot(exp_rows, up_w, preferred_element_type=jnp.float32)
    sigmoid_g = jax.nn.sigmoid(gate_pre)
    activated = (gate_pre * sigmoid_g * up_pre).astype(jnp.bfloat16)
    width_dims = (((1,), (1,)), ((), ()))
    d_act = lax.dot_general(exp_cot, down_w, width_dims, preferred_element_type=jnp.float32)
    d_gate = (d_act * up_pre * sigmoid_g * (1.0 + gate_pre * (1.0 - sigmoid_g))).astype(
        jnp.bfloat16
    )
    d_up = (d_act * gate_pre * sigmoid_g).astype(jnp.bfloat16)
    grads = expert_grads(exp_rows, exp_cot, activated, d_gate, d_up)
    partial_sum = lax.dot_general(d_gate, gate_w, width_dims, preferred_element_type=jnp.float32)
    partial_sum = partial_sum + lax.dot_general(
        d_up, up_w, width_dims, preferred_element_type=jnp.float32
    )
    if fused:
        mixer_cot, all_out = combine(
            partial_sum.astype(jnp.bfloat16).reshape(experts, capacity, model_width),
            picks,
            out_cot,
            mixer_out,
        )
    else:
        summed = lax.psum_scatter(
            partial_sum.reshape(experts, capacity, model_width), "tp", scatter_dimension=2, tiled=True
        )
        returned = lax.all_to_all(
            summed.astype(jnp.bfloat16), "sp", split_axis=0, concat_axis=0, tiled=True
        )
        col_count = model_width // narrow
        first_col = lax.axis_index("tp") * col_count
        back_flat = returned.reshape(experts * capacity, col_count)
        pair_back = back_flat[target].reshape(tok_rows, top_count, col_count).astype(jnp.float32)
        own_cols = lax.dynamic_slice_in_dim(out_cot, first_col, col_count, 1).astype(jnp.float32)
        cot_cols = (own_cols + jnp.sum(pair_back, axis=1)).astype(jnp.bfloat16)
        mixer_cot = lax.all_gather(cot_cols, "tp", axis=1, tiled=True)
    head_count = queries.shape[1] // DK
    head_ids = (lax.axis_index("tp") * head_count + jnp.arange(head_count, dtype=jnp.int32)).astype(
        jnp.float32
    )
    head_rates = decay_rates(head_ids, head_count * narrow, tok_rows * experts)
    positions = (lax.axis_index("sp") * tok_rows + jnp.arange(tok_rows, dtype=jnp.int32)).astype(
        jnp.float32
    )
    head_cot = jnp.dot(mixer_cot, out_proj, preferred_element_type=jnp.float32).reshape(
        tok_rows, head_count, DK
    )
    head_cot = (head_cot * position_norm(positions, head_rates)[:, :, None]).astype(jnp.bfloat16)
    span_count = tok_rows // SPAN
    span_shape = (span_count, SPAN, head_count, DK)
    span_query = queries.reshape(span_shape)
    span_key = keys.reshape(span_shape)
    span_value = values.reshape(span_shape)
    span_cot = head_cot.reshape(span_shape)
    key_scale = DK ** (-0.5)
    offsets = jnp.arange(SPAN, dtype=jnp.float32)
    distance = offsets[:, None] - offsets[None, :]
    decay_mat = jnp.where(
        distance[None] >= 0,
        jnp.exp(-head_rates[:, None, None] * jnp.maximum(distance, 0.0)[None]),
        0.0,
    )
    fwd_weights = (
        jnp.einsum("cihd,cjhd->chij", span_query, span_key, preferred_element_type=jnp.float32)
        * key_scale
        * decay_mat[None]
    ).astype(jnp.bfloat16)
    back_weights = (
        jnp.einsum("cihd,cjhd->chij", span_cot, span_value, preferred_element_type=jnp.float32)
        * decay_mat[None]
    ).astype(jnp.bfloat16)
    tail_decay = jnp.exp(-head_rates[None, :] * (SPAN - 1.0 - offsets)[:, None])
    lead_decay = jnp.exp(-head_rates[None, :] * (offsets + 1.0)[:, None])
    query_wide = span_query.astype(jnp.float32)
    key_wide = span_key.astype(jnp.float32)
    value_wide = span_value.astype(jnp.float32)
    cot_wide = span_cot.astype(jnp.float32)
    backs = jnp.einsum(
        "cihd,cihe->chde",
        query_wide * lead_decay[None, :, :, None],
        cot_wide,
        precision=lax.Precision.HIGHEST,
    )
    own_back = backs[0]
    ahead = jnp.arange(experts, dtype=jnp.int32) - lax.axis_index("sp") - 1
    reach = jnp.where(
        ahead[:, None] >= 0,
        jnp.exp(-head_rates[None, :] * (jnp.maximum(ahead, 0) * tok_rows)[:, None]),
        0.0,
    )
    if fused:
        packed = own_back.astype(jnp.bfloat16).reshape(head_count * DK // 2, 2 * DK)
        all_mixer, later = spread(
            mixer_cot, packed, jnp.repeat(reach.T, DK // 2, axis=0)
        )
        rev_states = later.reshape((1,) + own_back.shape)
        grad_proj = lax.dot_general(
            all_mixer.reshape(experts * tok_rows, model_width // experts),
            all_out.reshape(experts * tok_rows, mixer_out.shape[1]),
            (((0,), (0,)), ((), ())),
            preferred_element_type=jnp.float32,
        )
    else:
        all_backs = lax.all_gather(own_back, "sp")
        rev_states = jnp.sum(reach[:, :, None, None] * all_backs, axis=0)[None]
        grad_proj = lax.psum_scatter(
            lax.dot_general(
                mixer_cot, mixer_out, (((0,), (0,)), ((), ())), preferred_element_type=jnp.float32
            ),
            "sp",
            scatter_dimension=0,
            tiled=True,
        )
    fwd_stack = entry_states
    grad_q = key_scale * jnp.einsum(
        "chij,cjhd->cihd", back_weights, span_key, preferred_element_type=jnp.float32
    )
    grad_q = grad_q + lead_decay[None, :, :, None] * jnp.einsum(
        "chde,cihe->cihd", fwd_stack, cot_wide, precision=lax.Precision.HIGHEST
    )
    grad_k = jnp.einsum(
        "chij,cihd->cjhd", back_weights, span_query, preferred_element_type=jnp.float32
    )
    grad_k = key_scale * (
        grad_k
        + tail_decay[None, :, :, None]
        * jnp.einsum("chde,cjhe->cjhd", rev_states, value_wide, precision=lax.Precision.HIGHEST)
    )
    grad_v = jnp.einsum(
        "chij,cihe->cjhe", fwd_weights, span_cot, preferred_element_type=jnp.float32
    )
    grad_v = grad_v + key_scale * tail_decay[None, :, :, None] * jnp.einsum(
        "chde,cjhd->cjhe", rev_states, key_wide, precision=lax.Precision.HIGHEST
    )
    flat_shape = (tok_rows, head_count * DK)
    return (
        grads[0],
        grads[1],
        grads[2],
        grad_proj,
        grad_q.reshape(flat_shape).astype(jnp.bfloat16),
        grad_k.reshape(flat_shape).astype(jnp.bfloat16),
        grad_v.reshape(flat_shape).astype(jnp.bfloat16),
    )


def solution(mesh):
    placed = (
        P("sp", None),
        P("sp", None),
        P("sp", None),
        P("sp", None),
        P("sp", None, "tp"),
        P("sp", None, "tp"),
        P("sp", "tp", None),
        P(None, "tp"),
        P("sp", "tp"),
        P("sp", "tp"),
        P("sp", "tp"),
        P("sp", "tp"),
        P("sp", "tp", None, None),
    )
    return jax.shard_map(
        per_device,
        mesh=mesh,
        in_specs=placed,
        out_specs=(
            P("sp", None, "tp"),
            P("sp", None, "tp"),
            P("sp", "tp", None),
            P("sp", "tp"),
            P("sp", "tp"),
            P("sp", "tp"),
            P("sp", "tp"),
        ),
        check_vma=False,
    )
```

```python
import functools

import jax
import jax.numpy as jnp
from jax import lax
from jax.experimental import pallas as pl
from jax.experimental.pallas import tpu as pltpu
from jax.sharding import PartitionSpec as P

DK = 64
SPAN = 128
MESH = pl.DeviceIdType.MESH
VMEM = pl.BlockSpec(memory_space=pltpu.VMEM)


def seat(experts):
    me, tp = lax.axis_index("sp"), lax.axis_index("tp")
    core, row = tp % 2, tp // 2
    return me, tp, core, row, tp + 1 - 2 * core, (tp + 2) % 4


def greet(experts, me, tp_peers):
    barrier = pltpu.get_barrier_semaphore()
    for k in range(1, experts):
        pl.semaphore_signal(
            barrier, inc=1, device_id={"sp": (me + k) % experts}, device_id_type=MESH
        )
    for peer in tp_peers:
        pl.semaphore_signal(barrier, inc=1, device_id={"tp": peer}, device_id_type=MESH)
    pl.semaphore_wait(barrier, experts - 1 + len(tp_peers))


def send(src, dst, send_sem, recv_sem, target):
    copy = pltpu.make_async_remote_copy(
        src_ref=src,
        dst_ref=dst,
        send_sem=send_sem,
        recv_sem=recv_sem,
        device_id=target,
        device_id_type=MESH,
    )
    copy.start()
    return copy


def share_rows(experts, me, src, whole, own, s_r, r_r):
    mate = me + 1 - 2 * (me % 2)
    hops = []
    for k in range(1, experts // 2):
        peer = (me + 2 * k) % experts
        hops.append(send(src, whole.at[me], s_r.at[0, k], r_r.at[0, k], {"sp": peer}))
    relays = [send(src, whole.at[me], s_r.at[1, 0], r_r.at[1, 0], {"sp": mate})]
    local = pltpu.make_async_copy(src, whole.at[me], own)
    local.start()

    def relay():
        for k in range(1, experts // 2):
            hops[k - 1].wait_recv()
            held = whole.at[(me - 2 * k + experts) % experts]
            relays.append(send(held, held, s_r.at[1, k], r_r.at[1, k], {"sp": mate}))

    def arrive():
        local.wait()
        for copy in relays:
            copy.wait_recv()

    def drain():
        for copy in hops + relays:
            copy.wait_send()

    return relay, arrive, drain


def dispatch_kernel(
    experts,
    chosen,
    weight,
    rows_in,
    cot_in,
    out_rows,
    out_cot,
    rows,
    cot,
    own,
    s_sp, r_sp, s_y, r_y, s_c, r_c
):
    me, tp, core, row, mate, across = seat(experts)
    greet(experts, me, (mate, across))
    arrays = ((rows, out_rows), (cot, out_cot))
    share = out_rows.shape[2]

    def block(src, index):
        return src.at[pl.ds(pl.multiple_of(index * share, share), share)]

    far = {}
    for a, (src, dst) in enumerate(arrays):
        if a == 0:
            rows[...] = jnp.dot(
                chosen[...], rows_in[...], preferred_element_type=jnp.float32
            ).astype(jnp.bfloat16)
        else:
            picked = jnp.dot(chosen[...], cot_in[...], preferred_element_type=jnp.float32)
            cot[...] = (weight[...] * picked).astype(jnp.bfloat16)
        for k in range(1, experts):
            peer = (me + k) % experts
            far[a, k] = send(
                block(src, peer), dst.at[me, tp], s_sp.at[a, k], r_sp.at[a, k], {"sp": peer}
            )
    local = []
    for a, (src, dst) in enumerate(arrays):
        copy = pltpu.make_async_copy(block(src, me), dst.at[me, tp], own.at[a])
        copy.start()
        local.append(copy)
    for copy in local:
        copy.wait()
    side, near, relayed = {}, {}, {}

    def relay(k):
        origin = (me - k + experts) % experts
        for a, (src, dst) in enumerate(arrays):
            side[a, k].wait_recv()
            held = dst.at[origin, across]
            relayed[a, k] = send(held, held, s_c.at[a, 1, k], r_c.at[a, 1, k], {"tp": mate})

    for k in range(experts):
        origin = (me - k + experts) % experts
        for a, (src, dst) in enumerate(arrays):
            if k > 0:
                far[a, k].wait_recv()
            held = dst.at[origin, tp]
            side[a, k] = send(held, held, s_y.at[a, k], r_y.at[a, k], {"tp": across})
            near[a, k] = send(held, held, s_c.at[a, 0, k], r_c.at[a, 0, k], {"tp": mate})
        if k > 1:
            relay(k - 2)
    relay(experts - 2)
    relay(experts - 1)
    for copy in list(near.values()) + list(relayed.values()):
        copy.wait_recv()
    for group in (far, side, near, relayed):
        for copy in group.values():
            copy.wait_send()


def dispatch(chosen, weight, rows, cot, experts, narrow):
    width = rows.shape[1]
    share = chosen.shape[0] // experts
    held = pltpu.VMEM((experts * share, width), jnp.bfloat16)
    full = jax.ShapeDtypeStruct((experts, narrow, share, width), rows.dtype)
    sem = pltpu.SemaphoreType.DMA
    return pl.pallas_call(
        functools.partial(dispatch_kernel, experts),
        out_shape=(full, full),
        in_specs=[VMEM] * 4,
        out_specs=(VMEM, VMEM),
        scratch_shapes=[
            held,
            held,
            sem((2,)),
            sem((2, experts)),
            sem((2, experts)),
            sem((2, experts)),
            sem((2, experts)),
            sem((2, 2, experts)),
            sem((2, 2, experts)),
        ],
        compiler_params=pltpu.CompilerParams(collective_id=0, has_side_effects=True),
    )(chosen, weight, rows, cot)


def combine_kernel(
    experts,
    part,
    picks,
    own_cot,
    out_rows,
    mixer,
    all_out,
    near_buf,
    side_out,
    side_in,
    far_out,
    back,
    s_c,
    r_c,
    s_y,
    r_y,
    s_f,
    r_f,
    s_g,
    r_g,
    own,
    s_r,
    r_r,
):
    me, tp, core, row, mate, across = seat(experts)
    cols = part.shape[2] // 4

    def quarter(index):
        return pl.ds(pl.multiple_of(index * cols, cols), cols)

    greet(experts, me, (mate, across))
    order = list(range(1, experts)) + [0]
    relay, arrive, drain = share_rows(experts, me, out_rows, all_out, own.at[0], s_r, r_r)
    near, side, far = {}, {}, {}
    mate_core = 1 - core
    for k in order:
        dest = (me + k) % experts
        for half in range(2):
            near[k, half] = send(
                part.at[dest, :, quarter(half * 2 + mate_core)],
                near_buf.at[k, half],
                s_c.at[k, half],
                r_c.at[k, half],
                {"tp": mate},
            )
    for k in order:
        dest = (me + k) % experts
        near[k, 0].wait_recv()
        near[k, 1].wait_recv()
        side_out[k] = (
            part[dest, :, quarter(across)].astype(jnp.float32)
            + near_buf[k, 1 - row].astype(jnp.float32)
        ).astype(jnp.bfloat16)
        side[k] = send(side_out.at[k], side_in.at[k], s_y.at[k], r_y.at[k], {"tp": across})
    for k in order:
        dest = (me + k) % experts
        side[k].wait_recv()
        done = (
            part[dest, :, quarter(tp)].astype(jnp.float32)
            + near_buf[k, row].astype(jnp.float32)
            + side_in[k].astype(jnp.float32)
        ).astype(jnp.bfloat16)
        if k == 0:
            back[me] = done
        else:
            far_out[k] = done
            far[k] = send(far_out.at[k], back.at[me], s_f.at[k], r_f.at[k], {"sp": dest})
    relay()
    for k in range(1, experts):
        far[k].wait_recv()
    slots = back[...].reshape(experts * part.shape[1], cols)
    total = own_cot[:, quarter(tp)].astype(jnp.float32) + jnp.dot(
        picks[...], slots, preferred_element_type=jnp.float32
    )
    mixer[:, quarter(tp)] = total.astype(jnp.bfloat16)
    mine = mixer.at[:, quarter(tp)]
    other = mixer.at[:, quarter(across)]
    last = [
        send(mine, mine, s_g.at[0], r_g.at[0], {"tp": across}),
        send(mine, mine, s_g.at[1], r_g.at[1], {"tp": mate}),
    ]
    last[0].wait_recv()
    last.append(send(other, other, s_g.at[2], r_g.at[2], {"tp": mate}))
    last[1].wait_recv()
    last[2].wait_recv()
    arrive()
    drain()
    for group in (near.values(), side.values(), far.values(), last):
        for copy in group:
            copy.wait_send()


def combine(part, picks, own_cot, out_rows):
    experts, capacity, width = part.shape
    tok_rows = own_cot.shape[0]
    cols = width // 4
    sem = pltpu.SemaphoreType.DMA
    block = pltpu.VMEM((experts, capacity, cols), jnp.bfloat16)
    return pl.pallas_call(
        functools.partial(combine_kernel, experts),
        out_shape=(
            jax.ShapeDtypeStruct((tok_rows, width), jnp.bfloat16),
            jax.ShapeDtypeStruct((experts,) + out_rows.shape, out_rows.dtype),
        ),
        in_specs=[VMEM, VMEM, VMEM, VMEM],
        out_specs=(VMEM, VMEM),
        scratch_shapes=[
            pltpu.VMEM((experts, 2, capacity, cols), jnp.bfloat16),
            block,
            block,
            block,
            block,
            sem((experts, 2)),
            sem((experts, 2)),
            sem((experts,)),
            sem((experts,)),
            sem((experts,)),
            sem((experts,)),
            sem((3,)),
            sem((3,)),
            sem((1,)),
            sem((2, experts // 2)),
            sem((2, experts // 2)),
        ],
        compiler_params=pltpu.CompilerParams(collective_id=1, has_side_effects=True),
    )(part, picks, own_cot, out_rows)


def spread_kernel(
    experts, mixer, state, reach, all_mixer, later, all_state, own, s_m, r_m, s_r, r_r
):
    me = lax.axis_index("sp")
    cols = mixer.shape[1] // experts
    greet(experts, me, ())

    def block(index):
        return mixer.at[:, pl.ds(pl.multiple_of(index * cols, cols), cols)]

    relay, arrive, drain = share_rows(experts, me, state, all_state, own.at[0], s_r, r_r)
    copies = []
    for k in range(1, experts):
        peer = (me + k) % experts
        copies.append(
            send(block(peer), all_mixer.at[me], s_m.at[k], r_m.at[k], {"sp": peer})
        )
    local = pltpu.make_async_copy(block(me), all_mixer.at[me], own.at[1])
    local.start()
    relay()
    local.wait()
    arrive()
    total = jnp.zeros(later.shape, jnp.float32)
    for j in range(experts):
        total = total + reach[:, j : j + 1] * all_state[j].astype(jnp.float32)
    later[...] = total
    for copy in copies:
        copy.wait_recv()
    for copy in copies:
        copy.wait_send()
    drain()


def spread(mixer, state, reach):
    sem = pltpu.SemaphoreType.DMA
    tok_rows, width = mixer.shape
    experts = reach.shape[1]
    return pl.pallas_call(
        functools.partial(spread_kernel, experts),
        out_shape=(
            jax.ShapeDtypeStruct((experts, tok_rows, width // experts), mixer.dtype),
            jax.ShapeDtypeStruct(state.shape, jnp.float32),
        ),
        in_specs=[VMEM, VMEM, VMEM],
        out_specs=(VMEM, VMEM),
        scratch_shapes=[
            pltpu.VMEM((experts,) + state.shape, state.dtype),
            sem((2,)),
            sem((experts,)),
            sem((experts,)),
            sem((2, experts // 2)),
            sem((2, experts // 2)),
        ],
        compiler_params=pltpu.CompilerParams(collective_id=2, has_side_effects=True),
    )(mixer, state, reach)


def decay_rates(head_ids, head_count, token_count):
    half_count = head_count // 2
    fraction = jnp.minimum(head_ids, half_count) / half_count
    base_rate = jnp.exp(
        (1.0 - fraction) * jnp.log(1.0 / 32.0) + fraction * jnp.log(1.0 / token_count)
    )
    return base_rate * (1.0 + jnp.maximum(head_ids - half_count, 0.0) / half_count)


def position_norm(positions, head_rates):
    return jnp.sqrt(
        jnp.expm1(-2.0 * head_rates)[None, :]
        / jnp.expm1(-2.0 * head_rates[None, :] * (positions[:, None] + 1.0))
    )


def expert_grads(exp_rows, exp_cot, activated, d_gate, d_up):
    row_dims = (((0,), (0,)), ((), ()))
    grad_gate = lax.dot_general(
        exp_rows, d_gate, row_dims, preferred_element_type=jnp.float32
    ).astype(jnp.bfloat16)
    grad_up = lax.dot_general(exp_rows, d_up, row_dims, preferred_element_type=jnp.float32).astype(
        jnp.bfloat16
    )
    grad_down = lax.dot_general(
        activated, exp_cot, row_dims, preferred_element_type=jnp.float32
    ).astype(jnp.bfloat16)
    return (grad_gate[None], grad_up[None], grad_down[None])


def per_device(
    layer_input,
    out_cot,
    routes,
    route_weights,
    gate_weights,
    up_weights,
    down_weights,
    out_proj,
    queries,
    keys,
    values,
    mixer_out,
    entry_states,
):
    tok_rows, model_width = layer_input.shape
    experts = lax.axis_size("sp")
    narrow = lax.axis_size("tp")
    top_count = routes.shape[1]
    pair_count = tok_rows * top_count
    capacity = 2 * pair_count // experts
    flat_routes = routes.reshape(pair_count)
    onehot = (flat_routes[:, None] == jnp.arange(experts, dtype=jnp.int32)[None, :]).astype(
        jnp.int32
    )
    earlier = jnp.cumsum(onehot, axis=0) - onehot
    target = flat_routes * capacity + jnp.sum(earlier * onehot, axis=1)
    share = capacity // narrow
    first_row = lax.axis_index("tp") * share
    fused = narrow == 4 and experts % 2 == 0 and share % 16 == 0 and model_width % (experts * 128) == 0
    if fused:
        pair_slot = target.reshape(tok_rows, top_count)
        part_slot = (
            jnp.arange(experts, dtype=jnp.int32)[:, None] * capacity
            + first_row
            + jnp.arange(share, dtype=jnp.int32)[None, :]
        ).reshape(experts * share)
        hits = part_slot[:, None, None] == pair_slot[None]
        part_weight = jnp.sum(jnp.where(hits, route_weights[None], 0.0), axis=(1, 2))
        chosen = jnp.any(hits, axis=2).astype(jnp.bfloat16)
        got_rows, got_cot = dispatch(
            chosen, part_weight[:, None], layer_input, out_cot, experts, narrow
        )
        all_slots = jnp.arange(experts * capacity, dtype=jnp.int32)
        picks = jnp.any(pair_slot[:, :, None] == all_slots[None, None], axis=1).astype(
            jnp.bfloat16
        )
    else:
        owner_tok = jnp.arange(pair_count, dtype=jnp.int32) // top_count
        slot_tok = jnp.full((experts * capacity,), tok_rows, jnp.int32).at[target].set(owner_tok)
        slot_weight = (
            jnp.zeros((experts * capacity,), jnp.float32)
            .at[target]
            .set(route_weights.reshape(pair_count))
        )
        blank_row = jnp.zeros((1, model_width), jnp.bfloat16)
        sent_rows = jnp.concatenate([layer_input, blank_row], 0)[slot_tok].reshape(
            experts, capacity, model_width
        )
        picked_cot = jnp.concatenate([out_cot, blank_row], 0)[slot_tok]
        sent_cot = (
            (slot_weight[:, None] * picked_cot.astype(jnp.float32))
            .astype(jnp.bfloat16)
            .reshape(experts, capacity, model_width)
        )
        part_rows = lax.dynamic_slice_in_dim(sent_rows, first_row, share, 1)
        part_cot = lax.dynamic_slice_in_dim(sent_cot, first_row, share, 1)
        got_rows, got_cot = (
            lax.all_to_all(part_rows, "sp", split_axis=0, concat_axis=0, tiled=True),
            lax.all_to_all(part_cot, "sp", split_axis=0, concat_axis=0, tiled=True),
        )
        got_rows, got_cot = (
            lax.all_gather(got_rows, "tp", axis=1, tiled=True),
            lax.all_gather(got_cot, "tp", axis=1, tiled=True),
        )
    exp_rows = got_rows.reshape(experts * capacity, model_width)
    exp_cot = got_cot.reshape(experts * capacity, model_width)
    gate_w = gate_weights[0]
    up_w = up_weights[0]
    down_w = down_weights[0]
    gate_pre = jnp.dot(exp_rows, gate_w, preferred_element_type=jnp.float32)
    up_pre = jnp.dot(exp_rows, up_w, preferred_element_type=jnp.float32)
    sigmoid_g = jax.nn.sigmoid(gate_pre)
    activated = (gate_pre * sigmoid_g * up_pre).astype(jnp.bfloat16)
    width_dims = (((1,), (1,)), ((), ()))
    d_act = lax.dot_general(exp_cot, down_w, width_dims, preferred_element_type=jnp.float32)
    d_gate = (d_act * up_pre * sigmoid_g * (1.0 + gate_pre * (1.0 - sigmoid_g))).astype(
        jnp.bfloat16
    )
    d_up = (d_act * gate_pre * sigmoid_g).astype(jnp.bfloat16)
    grads = expert_grads(exp_rows, exp_cot, activated, d_gate, d_up)
    partial_sum = lax.dot_general(d_gate, gate_w, width_dims, preferred_element_type=jnp.float32)
    partial_sum = partial_sum + lax.dot_general(
        d_up, up_w, width_dims, preferred_element_type=jnp.float32
    )
    if fused:
        mixer_cot, all_out = combine(
            partial_sum.astype(jnp.bfloat16).reshape(experts, capacity, model_width),
            picks,
            out_cot,
            mixer_out,
        )
    else:
        summed = lax.psum_scatter(
            partial_sum.reshape(experts, capacity, model_width), "tp", scatter_dimension=2, tiled=True
        )
        returned = lax.all_to_all(
            summed.astype(jnp.bfloat16), "sp", split_axis=0, concat_axis=0, tiled=True
        )
        col_count = model_width // narrow
        first_col = lax.axis_index("tp") * col_count
        back_flat = returned.reshape(experts * capacity, col_count)
        pair_back = back_flat[target].reshape(tok_rows, top_count, col_count).astype(jnp.float32)
        own_cols = lax.dynamic_slice_in_dim(out_cot, first_col, col_count, 1).astype(jnp.float32)
        cot_cols = (own_cols + jnp.sum(pair_back, axis=1)).astype(jnp.bfloat16)
        mixer_cot = lax.all_gather(cot_cols, "tp", axis=1, tiled=True)
    head_count = queries.shape[1] // DK
    head_ids = (lax.axis_index("tp") * head_count + jnp.arange(head_count, dtype=jnp.int32)).astype(
        jnp.float32
    )
    head_rates = decay_rates(head_ids, head_count * narrow, tok_rows * experts)
    positions = (lax.axis_index("sp") * tok_rows + jnp.arange(tok_rows, dtype=jnp.int32)).astype(
        jnp.float32
    )
    head_cot = jnp.dot(mixer_cot, out_proj, preferred_element_type=jnp.float32).reshape(
        tok_rows, head_count, DK
    )
    head_cot = (head_cot * position_norm(positions, head_rates)[:, :, None]).astype(jnp.bfloat16)
    span_count = tok_rows // SPAN
    span_shape = (span_count, SPAN, head_count, DK)
    span_query = queries.reshape(span_shape)
    span_key = keys.reshape(span_shape)
    span_value = values.reshape(span_shape)
    span_cot = head_cot.reshape(span_shape)
    key_scale = DK ** (-0.5)
    offsets = jnp.arange(SPAN, dtype=jnp.float32)
    distance = offsets[:, None] - offsets[None, :]
    decay_mat = jnp.where(
        distance[None] >= 0,
        jnp.exp(-head_rates[:, None, None] * jnp.maximum(distance, 0.0)[None]),
        0.0,
    )
    fwd_weights = (
        jnp.einsum("cihd,cjhd->chij", span_query, span_key, preferred_element_type=jnp.float32)
        * key_scale
        * decay_mat[None]
    ).astype(jnp.bfloat16)
    back_weights = (
        jnp.einsum("cihd,cjhd->chij", span_cot, span_value, preferred_element_type=jnp.float32)
        * decay_mat[None]
    ).astype(jnp.bfloat16)
    tail_decay = jnp.exp(-head_rates[None, :] * (SPAN - 1.0 - offsets)[:, None])
    lead_decay = jnp.exp(-head_rates[None, :] * (offsets + 1.0)[:, None])
    query_wide = span_query.astype(jnp.float32)
    key_wide = span_key.astype(jnp.float32)
    value_wide = span_value.astype(jnp.float32)
    cot_wide = span_cot.astype(jnp.float32)
    backs = jnp.einsum(
        "cihd,cihe->chde",
        query_wide * lead_decay[None, :, :, None],
        cot_wide,
        precision=lax.Precision.HIGHEST,
    )
    own_back = backs[0]
    ahead = jnp.arange(experts, dtype=jnp.int32) - lax.axis_index("sp") - 1
    reach = jnp.where(
        ahead[:, None] >= 0,
        jnp.exp(-head_rates[None, :] * (jnp.maximum(ahead, 0) * tok_rows)[:, None]),
        0.0,
    )
    if fused:
        packed = own_back.astype(jnp.bfloat16).reshape(head_count * DK // 2, 2 * DK)
        all_mixer, later = spread(
            mixer_cot, packed, jnp.repeat(reach.T, DK // 2, axis=0)
        )
        rev_states = later.reshape((1,) + own_back.shape)
        grad_proj = lax.dot_general(
            all_mixer.reshape(experts * tok_rows, model_width // experts),
            all_out.reshape(experts * tok_rows, mixer_out.shape[1]),
            (((0,), (0,)), ((), ())),
            preferred_element_type=jnp.float32,
        )
    else:
        all_backs = lax.all_gather(own_back, "sp")
        rev_states = jnp.sum(reach[:, :, None, None] * all_backs, axis=0)[None]
        grad_proj = lax.psum_scatter(
            lax.dot_general(
                mixer_cot, mixer_out, (((0,), (0,)), ((), ())), preferred_element_type=jnp.float32
            ),
            "sp",
            scatter_dimension=0,
            tiled=True,
        )
    fwd_stack = entry_states
    grad_q = key_scale * jnp.einsum(
        "chij,cjhd->cihd", back_weights, span_key, preferred_element_type=jnp.float32
    )
    grad_q = grad_q + lead_decay[None, :, :, None] * jnp.einsum(
        "chde,cihe->cihd", fwd_stack, cot_wide, precision=lax.Precision.HIGHEST
    )
    grad_k = jnp.einsum(
        "chij,cihd->cjhd", back_weights, span_query, preferred_element_type=jnp.float32
    )
    grad_k = key_scale * (
        grad_k
        + tail_decay[None, :, :, None]
        * jnp.einsum("chde,cjhe->cjhd", rev_states, value_wide, precision=lax.Precision.HIGHEST)
    )
    grad_v = jnp.einsum(
        "chij,cihe->cjhe", fwd_weights, span_cot, preferred_element_type=jnp.float32
    )
    grad_v = grad_v + key_scale * tail_decay[None, :, :, None] * jnp.einsum(
        "chde,cjhd->cjhe", rev_states, key_wide, precision=lax.Precision.HIGHEST
    )
    flat_shape = (tok_rows, head_count * DK)
    return (
        grads[0],
        grads[1],
        grads[2],
        grad_proj,
        grad_q.reshape(flat_shape).astype(jnp.bfloat16),
        grad_k.reshape(flat_shape).astype(jnp.bfloat16),
        grad_v.reshape(flat_shape).astype(jnp.bfloat16),
    )


def solution(mesh):
    placed = (
        P("sp", None),
        P("sp", None),
        P("sp", None),
        P("sp", None),
        P("sp", None, "tp"),
        P("sp", None, "tp"),
        P("sp", "tp", None),
        P(None, "tp"),
        P("sp", "tp"),
        P("sp", "tp"),
        P("sp", "tp"),
        P("sp", "tp"),
        P("sp", "tp", None, None),
    )
    return jax.shard_map(
        per_device,
        mesh=mesh,
        in_specs=placed,
        out_specs=(
            P("sp", None, "tp"),
            P("sp", None, "tp"),
            P("sp", "tp", None),
            P("sp", "tp"),
            P("sp", "tp"),
            P("sp", "tp"),
            P("sp", "tp"),
        ),
        check_vma=False,
    )
```
